32 devices in a mesh: sp: 8 (over z, x), tp: 4 (over y, core).
Axes of the slice: x: 2, y: 2, z: 4, core: 2. Of those that a mesh axis runs over, the one named last changes fastest.
Arguments:
- tokens: bfloat16 [8192, 2048], P('sp'), may hold values from -8 to 8
- norm_gain: float32 [2048], replicated, may hold values from 0.1 to 1.9
- query_weight: bfloat16 [2048, 512], P(None, 'tp'), may hold values from -40 to 40
- key_weight: bfloat16 [2048, 256], P(None, 'tp'), may hold values from -1 to 1
- value_weight: bfloat16 [2048, 256], P(None, 'tp'), may hold values from -0.125 to 0.125
- sink_logits: float32 [8], P('tp'), may hold values from 1 to 6
- conv_in_weight: bfloat16 [2048, 512], P(None, 'tp'), may hold values from -0.125 to 0.125
- conv_gate_weight: bfloat16 [2048, 512], P(None, 'tp'), may hold values from -0.125 to 0.125
- conv_taps: bfloat16 [31, 512], replicated, may hold values from -1 to 1
- conv_gain: float32 [512], replicated, may hold values from 0.1 to 1.9
- point_weight: bfloat16 [512, 512], replicated, may hold values from -0.25 to 0.25
- output_gain: float32 [1024], replicated, may hold values from 0.1 to 1.9
- output_weight: bfloat16 [1024, 2048], P('sp'), may hold values from -0.1875 to 0.1875
Outputs:
- mixed_output: bfloat16 [8192, 2048], P(('sp', 'tp'))
The draws below stay inside these ranges and needn't reach their ends.
All inputs are finite; a program needn't handle non-finite values.
Results may differ from the reference program's by a relative error of at most 0.0087.
Values may be sent and summed in bfloat16 or wider, within the bound.
A program may use at most 64 MiB of HBM per device.

```python
import jax
import jax.numpy as jnp
from jax import lax

D = 2048
HEADS = 8
KV_HEADS = 4
HEAD_DIM = 64
CHANNELS = 512
WINDOW = 128
CONV_WIDTH = 31
TOKENS = 8192
MIX = 1024


def base_query(key):
    gaussian = jax.random.normal(jax.random.fold_in(key, 501), (D, HEADS * HEAD_DIM), jnp.float32)
    return jnp.clip(gaussian, -6.0, 6.0) * D ** (-0.5)


def draw_query_weight(key, part):
    unscaled = base_query(key)
    return unscaled.astype(jnp.bfloat16)


def draw_key_weight(key, part):
    fresh_noise = jax.random.normal(jax.random.fold_in(key, 502), (D, KV_HEADS * HEAD_DIM), jnp.float32)
    fresh_noise = jnp.clip(fresh_noise, -6.0, 6.0) * D ** (-0.5)
    return fresh_noise.astype(jnp.bfloat16)


def draw_tokens(key, part):
    shape_rows = (TOKENS, D)
    gaussian = jnp.clip(jax.random.normal(jax.random.fold_in(key, 601), shape_rows, jnp.float32), -6.0, 6.0)
    return gaussian.astype(jnp.bfloat16)


def block_levels(key, extent, split, low, top_value):
    def one(dim, shards_of):
        heights = jax.random.uniform(jax.random.fold_in(jax.random.fold_in(key, 6), dim), (shards_of,), jnp.float32, low / len(split), top_value / len(split))
        return jnp.repeat(jnp.exp(heights), extent[dim] // shards_of).reshape((-1,) + (1,) * (len(extent) - dim - 1))

    factor_of = one(*split[0])
    for cut in split[1:]:
        factor_of = factor_of * one(*cut)
    return factor_of


def scatter_about(key, dims, deviation, reach, cuts=(), kind=jnp.bfloat16):
    entries = deviation * jax.random.normal(key, dims, jnp.float32)
    if cuts:
        entries = entries * block_levels(key, dims, cuts, -0.22, 0.18)
    return jnp.clip(entries, -reach, reach).astype(kind)


def setup_inputs(seed: int = 0) -> dict:
    seeds = jax.random.split(jax.random.key(seed), 14)
    return {
        "tokens": draw_tokens(jax.random.fold_in(seeds[13], 71), 0),
        "norm_gain": jnp.clip(1.0 + 0.18 * jax.random.normal(seeds[1], (D,), jnp.float32), 0.1, 1.9),
        "query_weight": draw_query_weight(jax.random.fold_in(seeds[13], 71), 0),
        "key_weight": draw_key_weight(jax.random.fold_in(seeds[13], 71), 0),
        "value_weight": scatter_about(seeds[4], (D, KV_HEADS * HEAD_DIM), D ** -0.5, 0.125, ((1, 4),)),
        "sink_logits": jnp.clip(1.0 + 5.0 * jax.random.uniform(seeds[5], (HEADS,), jnp.float32) ** block_levels(seeds[5], (HEADS,), ((0, 4),), -0.2, 0.2), 1.0, 6.0),
        "conv_in_weight": scatter_about(seeds[6], (D, CHANNELS), D ** -0.5, 0.125, ((1, 4),)),
        "conv_gate_weight": scatter_about(seeds[7], (D, CHANNELS), D ** -0.5, 0.125, ((1, 4),)),
        "conv_taps": scatter_about(seeds[8], (CONV_WIDTH, CHANNELS), CONV_WIDTH ** -0.5, 1.0),
        "conv_gain": jnp.clip(1.0 + 0.18 * jax.random.normal(seeds[9], (CHANNELS,), jnp.float32), 0.1, 1.9),
        "point_weight": scatter_about(seeds[10], (CHANNELS, CHANNELS), CHANNELS ** -0.5, 0.25),
        "output_gain": jnp.clip(1.0 + 0.18 * jax.random.normal(seeds[11], (MIX,), jnp.float32), 0.1, 1.9),
        "output_weight": scatter_about(seeds[12], (MIX, D), MIX ** -0.5, 0.1875, ((0, 8),)),
    }


NORM_EPSILON = 1e-06
MASKED_SCORE = -1e+30

def rms_rows(values, scale_gain):
    return values * lax.rsqrt(lax.optimization_barrier(jnp.mean(values * values, axis=-1, keepdims=True)) + NORM_EPSILON) * scale_gain

def depthwise(current, earlier_rows, tap_weights):
    extended = jnp.concatenate([earlier_rows, current], axis=0).astype(jnp.float32)
    tap_floats = tap_weights.astype(jnp.float32)
    row_count = current.shape[0]
    result = jnp.zeros(current.shape, jnp.float32)
    for tap_index in range(CONV_WIDTH):
        result = result + tap_floats[tap_index] * extended[tap_index:tap_index + row_count]
    return lax.optimization_barrier(result.astype(jnp.bfloat16))

def layer_activate(conv_rows, channel_gain):
    widened = conv_rows.astype(jnp.float32)
    centered = widened - lax.optimization_barrier(jnp.mean(widened, axis=-1, keepdims=True))
    scaled = centered * lax.rsqrt(lax.optimization_barrier(jnp.mean(centered * centered, axis=-1, keepdims=True)) + NORM_EPSILON) * channel_gain
    return jax.nn.silu(scaled).astype(jnp.bfloat16)

def merge_groups(attended, pointwise, output_gain):
    head_width = attended.shape[1]
    return jnp.concatenate([rms_rows(attended.astype(jnp.float32), output_gain[:head_width]), rms_rows(pointwise, output_gain[head_width:])], axis=1).astype(jnp.bfloat16)

def reference(tokens, norm_gain, query_weight, key_weight, value_weight, sink_logits, conv_in_weight, conv_gate_weight, conv_taps, conv_gain, point_weight, output_gain, output_weight):
    normed = rms_rows(tokens.astype(jnp.float32), norm_gain).astype(jnp.bfloat16)
    queries = jnp.dot(normed, query_weight, preferred_element_type=jnp.float32).astype(jnp.bfloat16)
    key_part = jnp.dot(normed, key_weight, preferred_element_type=jnp.float32).astype(jnp.bfloat16)
    value_part = jnp.dot(normed, value_weight, preferred_element_type=jnp.float32).astype(jnp.bfloat16)
    conv_in = jnp.dot(normed, conv_in_weight, preferred_element_type=jnp.float32)
    conv_gate = jnp.dot(normed, conv_gate_weight, preferred_element_type=jnp.float32)
    gated_rows = (conv_in * jax.nn.sigmoid(conv_gate)).astype(jnp.bfloat16)
    group_size = HEADS // KV_HEADS
    block_count = TOKENS // WINDOW
    head_queries = jnp.transpose(queries.reshape(TOKENS, KV_HEADS, group_size, HEAD_DIM), (1, 0, 2, 3))
    head_keys = jnp.transpose(key_part.reshape(TOKENS, KV_HEADS, HEAD_DIM), (1, 0, 2))
    head_values = jnp.transpose(value_part.reshape(TOKENS, KV_HEADS, HEAD_DIM), (1, 0, 2))
    head_sinks = sink_logits.reshape(KV_HEADS, group_size)
    query_index = lax.broadcasted_iota(jnp.int32, (WINDOW, 2 * WINDOW), 0)
    key_index = lax.broadcasted_iota(jnp.int32, (WINDOW, 2 * WINDOW), 1)
    distance = WINDOW + query_index - key_index
    in_window = (distance >= 0) & (distance < WINDOW)
    block_start = jnp.arange(block_count, dtype=jnp.int32) * WINDOW - WINDOW
    allowed = in_window[None] & (block_start[:, None, None] + key_index[None] >= 0)

    def banded(rows_in):
        padding = jnp.zeros((WINDOW, HEAD_DIM), rows_in.dtype)
        extended = jnp.concatenate([padding, rows_in], axis=0).reshape(block_count + 1, WINDOW, HEAD_DIM)
        return jnp.concatenate([extended[:-1], extended[1:]], axis=1)

    def one_head(operands):
        group_queries, group_keys, group_values, group_sinks = operands
        blocked = group_queries.reshape(block_count, WINDOW, group_size, HEAD_DIM).astype(jnp.float32)
        scores = jnp.einsum('nqgd,njd->ngqj', blocked, banded(group_keys).astype(jnp.float32)) * HEAD_DIM ** (-0.5)
        scores = jnp.where(allowed[:, None], scores, MASKED_SCORE)
        sink_logit = group_sinks[None, :, None, None]
        row_peak = jnp.maximum(lax.optimization_barrier(jnp.max(scores, axis=-1, keepdims=True)), sink_logit)
        raised = jnp.exp(scores - row_peak)
        denominator = lax.optimization_barrier(jnp.sum(raised, axis=-1, keepdims=True)) + jnp.exp(sink_logit - row_peak)
        weights = (raised / denominator).astype(jnp.bfloat16)
        attended = jnp.einsum('ngqj,njd->nqgd', weights.astype(jnp.float32), banded(group_values).astype(jnp.float32))
        return attended.astype(jnp.bfloat16)
    per_head = lax.map(one_head, (head_queries, head_keys, head_values, head_sinks))
    attended = jnp.transpose(per_head, (1, 2, 0, 3, 4)).reshape(TOKENS, HEADS * HEAD_DIM)
    earlier_rows = jnp.zeros((CONV_WIDTH - 1, CHANNELS), jnp.bfloat16)
    convolved = depthwise(gated_rows, earlier_rows, conv_taps)
    activated = layer_activate(convolved, conv_gain)
    pointwise = jnp.dot(activated, point_weight, preferred_element_type=jnp.float32)
    merged = merge_groups(attended, pointwise, output_gain)
    return jnp.dot(merged, output_weight, preferred_element_type=jnp.float32).astype(jnp.bfloat16)
```

```python
import functools

import jax
import jax.numpy as jnp
from jax import lax
from jax.experimental import pallas as pl
from jax.experimental.pallas import tpu as pltpu
from jax.sharding import PartitionSpec as P

HEAD_DIM = 64
WINDOW = 128
CONV_WIDTH = 31
HALO = 32
EPS = 1e-06
MASKED = -1e30
F32 = jnp.float32
BF16 = jnp.bfloat16
MESH = pl.DeviceIdType.MESH


def kernel(
    S, T,
    tok_hbm, ng_hbm, qw, kw, vw, sink_hbm, iw, gw, taps_hbm, cg_hbm, pw_hbm, og_hbm, ow_hbm,
    out,
    tok, wcat, kvs, pw, wfull, qb, kvb, g, a, ar, gr, ext, conv, act, mg, acc, theirs, ng, sink, taps, cg, og,
    lsem, wsend, wrecv, hsend, hrecv, asend, arecv, gsend, grecv, msend, mrecv, osend, orecv,
):
    s, t = lax.axis_index("sp"), lax.axis_index("tp")
    R, D = tok.shape
    Q = R // T
    Kl = ow_hbm.shape[0]
    Y, Z = T // 2, S // 2
    z, x = s // 2, lax.rem(s, 2)
    y, c = t // 2, lax.rem(t, 2)
    CC = g.shape[1]
    HW = a.shape[1]

    half, wide = D // 2, D // 4
    part, narrow = wide // 2, wide // Y
    own = pl.ds(pl.multiple_of(s * Kl, Kl), Kl)
    own_half = ow_hbm.at[:, pl.ds(pl.multiple_of(c * half, half), half)]
    loads = [pltpu.make_async_copy(own_half, wfull.at[own], lsem.at[0])]
    loads += [
        pltpu.make_async_copy(qw, wcat.at[:, 0:HW], lsem.at[1]),
        pltpu.make_async_copy(kw, kvs.at[0 : kw.shape[0]], lsem.at[2]),
        pltpu.make_async_copy(vw, kvs.at[kw.shape[0] : 2 * kw.shape[0]], lsem.at[3]),
        pltpu.make_async_copy(iw, wcat.at[:, 2 * HW : 2 * HW + CC], lsem.at[4]),
        pltpu.make_async_copy(gw, wcat.at[:, 2 * HW + CC : 2 * HW + 2 * CC], lsem.at[5]),
        pltpu.make_async_copy(pw_hbm, pw, lsem.at[6]),
    ]
    tloads = [
        pltpu.make_async_copy(tok_hbm.at[q * Q : (q + 1) * Q], tok.at[q * Q : (q + 1) * Q], lsem.at[7 + q])
        for q in range(T)
    ]
    bar = pltpu.get_barrier_semaphore()

    def hello(ds_, dt_):
        pl.semaphore_signal(bar, inc=1, device_id=(ds_, dt_), device_id_type=MESH)

    for d in range(1, T):
        hello(s, lax.rem(t + d, T))
    hello(s + 1 - 2 * x, t)
    peers = T
    for step in (1, 2):
        @pl.when(s >= step)
        def _():
            hello(s - step, t)

        @pl.when(s + step < S)
        def _():
            hello(s + step, t)

        peers = peers + jnp.where(s >= step, 1, 0) + jnp.where(s + step < S, 1, 0)
    small = [
        pltpu.make_async_copy(src, dst, lsem.at[7 + T + i])
        for i, (src, dst) in enumerate(
            ((ng_hbm, ng), (sink_hbm, sink), (taps_hbm, taps), (cg_hbm, cg), (og_hbm, og))
        )
    ]
    loads[0].start()
    small[0].start()
    tloads[T - 1].start()
    for i in range(1, 6):
        loads[i].start()
    for q in range(T - 2, -1, -1):
        tloads[q].start()
    loads[6].start()
    for copy in small[1:]:
        copy.start()


    pl.semaphore_wait(bar, peers)

    other_x = s + 1 - 2 * x
    sib = y * 2 + 1 - c
    W0, W1, N = 0, 1, 2 + y
    M = [2 + lax.rem(y + k, Y) for k in range(1, Y)]
    groups = {}
    count = [0]
    conds = {}

    def cond_of(name, f):
        if name not in conds:
            conds[name] = f()
        return name

    def when(cond, f):
        if cond is None:
            f()
        else:
            pl.when(conds[cond])(f)

    front = z < Z // 2
    m = jnp.where(front, z, Z - 1 - z)

    def plane(r):
        spot = jnp.where(r <= 2 * m, m + (r // 2 if r % 2 == 0 else -(r + 1) // 2), r)
        return jnp.where(front, spot, Z - 1 - spot)

    def mine(r):
        return plane(r) * 2 + x

    def other(r):
        return plane(r) * 2 + 1 - x

    def onward(r):
        far = plane(r)
        return jnp.where(far < z, z + 1 < Z, z >= 1)

    def finishing(r):
        far = plane(r)
        up = (far == 0) & (z + 1 < Z) & (z + 1 >= Z // 2)
        down = (far == Z - 1) & (z >= 1) & (z - 1 < Z // 2)
        return up | down

    def unit(sh, u):
        rows = pl.ds(pl.multiple_of(sh * Kl, Kl), Kl)
        if isinstance(u, int) and u < 2:
            return wfull.at[rows, u * part : (u + 1) * part]
        return wfull.at[rows, pl.ds(pl.multiple_of(wide + (u - 2) * narrow, narrow), narrow)]

    def push(cond, src, dst, width, rsem, ds_, dt_):
        group = groups.setdefault(cond, [])
        if not group or group[-1][1] + width > half:
            group.append([count[0], 0])
            count[0] += 1
        group[-1][1] += width
        sem = wsend.at[group[-1][0]]

        def go():
            pltpu.make_async_remote_copy(
                src_ref=src, dst_ref=dst, send_sem=sem, recv_sem=rsem,
                device_id=(ds_, dt_), device_id_type=MESH,
            ).start()

        when(cond, go)

    def drain():
        for cond, group in groups.items():
            def wait(group=group):
                for i, width in group:
                    ref = wfull.at[0:Kl, 0:width]
                    pltpu.make_async_copy(ref, ref, wsend.at[i]).wait()

            when(cond, wait)

    def send(cond, sh, u, ds_, dt_):
        ref = unit(sh, u)
        width = part if isinstance(u, int) and u < 2 else narrow
        push(cond, ref, ref, width, wrecv.at[sh, u], ds_, dt_)

    def got(cond, sh, u):
        ref = unit(sh, u)
        when(cond, lambda: pltpu.make_async_copy(ref, ref, wrecv.at[sh, u]).wait())

    def to_x(cond, sh, u):
        send(cond, sh, u, other_x, t)

    def to_y(cond, sh):
        for k in range(1, Y):
            send(cond, sh, N, s, lax.rem(y + k, Y) * 2 + c)

    def z_out(sh, u):
        send(cond_of("up", lambda: z + 1 < Z), sh, u, s + 2, t)
        send(cond_of("down", lambda: z >= 1), sh, u, s - 2, t)

    def relay(r, u, oth=False):
        if not oth and not any(u is v for v in M):
            cond = cond_of(("onward", r), lambda: onward(r))
        else:
            cond = cond_of(("finishing", r), lambda: finishing(r))
        step = jnp.where(plane(r) < z, 2, -2)
        send(cond, other(r) if oth else mine(r), u, s + step, t)

    def plane_n(r, cond=None):
        got(cond, mine(r), N)
        if r < Z - 1:
            to_y(cond, mine(r))
            to_x(cond, mine(r), N)

    def plane_w(r, u, cond=None):
        got(cond, mine(r), u)
        to_x(cond, mine(r), u)

    def other_n(r, cond=None):
        got(cond, other(r), N)
        if r > 0:
            to_y(cond, other(r))

    def other_w(r, cond=None):
        got(cond, other(r), W0)
        got(cond, other(r), W1)

    def across(sh, cond=None):
        for u in M:
            got(cond, sh, u)

    def rest(r):
        other_w(r)
        if r != 1:
            across(mine(r))
        across(other(r))

    def inner():
        for r in range(3, last):
            for u in (N, W0, W1):
                (plane_n(r) if u is N else plane_w(r, u))
                relay(r, u)
            other_n(r)
            relay(r, N, True)
            across(mine(r))
            for u in M:
                relay(r, u)
            other_w(r)
            across(other(r))

    mid = cond_of("mid", lambda: (z > 0) & (z < Z - 1))
    end = cond_of("end", lambda: (z == 0) | (z == Z - 1))
    last = Z - 1

    loads[0].wait()
    for u in (N, W0):
        z_out(s, u)
        to_x(None, s, u)

    for i in range(1, 6):
        loads[i].wait()
    small[0].wait()
    wcat[:, HW : 2 * HW] = kvs[...].T

    def send_gated(q):
        rows = pl.ds(q * Q, HALO + Q)

        @pl.when(t != q)
        def _():
            pltpu.make_async_remote_copy(
                src_ref=g.at[rows], dst_ref=gr.at[t], send_sem=gsend.at[q], recv_sem=grecv.at[t],
                device_id=(s, q), device_id_type=MESH,
            ).start()

    def halo(ref, n, i):
        return pltpu.make_async_remote_copy(
            src_ref=ref.at[pl.ds(R, n)], dst_ref=ref.at[pl.ds(0, n)],
            send_sem=hsend.at[i], recv_sem=hrecv.at[i],
            device_id=(lax.rem(s + 1, S), t), device_id_type=MESH,
        )

    for q in range(T - 1, -1, -1):
        tloads[q].wait()
        xs = tok[q * Q : (q + 1) * Q, :].astype(F32)
        scale = lax.rsqrt(jnp.mean(xs * xs, axis=-1, keepdims=True) + EPS)
        normed = (xs * scale * ng[...]).astype(BF16)
        p = jnp.dot(normed, wcat[...], preferred_element_type=F32)
        qb[q * Q : (q + 1) * Q, :] = (p[:, :HW] * HEAD_DIM ** (-0.5)).astype(BF16)
        kvb[WINDOW + q * Q : WINDOW + (q + 1) * Q, :] = p[:, HW : 2 * HW].astype(BF16)
        g[HALO + q * Q : HALO + (q + 1) * Q, :] = (
            p[:, 2 * HW : 2 * HW + CC] * jax.nn.sigmoid(p[:, 2 * HW + CC :])
        ).astype(BF16)
        if q == T - 1:
            @pl.when(s + 1 < S)
            def _():
                halo(kvb, WINDOW, 0).start()
                halo(g, HALO, 1).start()
            z_out(s, W1)
            to_x(None, s, W1)
        else:
            send_gated(q + 1)
        if q == 1:
            plane_n(1)
            plane_n(2, mid)
            relay(2, N)

    small[1].wait()
    row = lax.broadcasted_iota(jnp.int32, (2 * WINDOW, 2 * WINDOW), 0)
    col = lax.broadcasted_iota(jnp.int32, (2 * WINDOW, 2 * WINDOW), 1)
    dist = WINDOW + lax.rem(row, WINDOW) - col
    inside = (dist >= 0) & (dist < WINDOW)
    head = lax.broadcasted_iota(jnp.int32, (2 * WINDOW, 1), 0) < WINDOW
    sinks = jnp.where(head, sink[0], sink[1])
    for copy in small[2:]:
        copy.wait()
    for i in range(T):
        if i < T - 2:
            q = 1 + lax.rem(t + i, T - 1)
        elif i == T - 2:
            q = (T - t) // T * (T - 1)
        else:
            q = t
        for b in range(Q // WINDOW):
            base = pl.multiple_of(q * Q + b * WINDOW, WINDOW)
            rows = qb[pl.ds(base, WINDOW), :]
            kv = kvb[pl.ds(base, 2 * WINDOW), :]
            q2 = jnp.concatenate([rows[:, :HEAD_DIM], rows[:, HEAD_DIM:]], axis=0)
            sc = lax.dot_general(
                q2, kv[:, :HEAD_DIM], (((1,), (1,)), ((), ())), preferred_element_type=F32
            )
            low = jnp.where((s == 0) & (base == 0), WINDOW, 0)
            sc = jnp.where(inside & (col >= low), sc, MASKED)
            top = jnp.maximum(jnp.max(sc, axis=-1, keepdims=True), sinks)
            e = jnp.exp(sc - top)
            den = jnp.sum(e, axis=-1, keepdims=True) + jnp.exp(sinks - top)
            w = (e * (1.0 / den)).astype(BF16)
            o = jnp.dot(w, kv[:, HEAD_DIM:], preferred_element_type=F32).astype(BF16)
            a[pl.ds(base, WINDOW), :] = jnp.concatenate([o[:WINDOW], o[WINDOW:]], axis=1)
        if i < T - 1:
            pltpu.make_async_remote_copy(
                src_ref=a.at[pl.ds(pl.multiple_of(q * Q, Q), Q)], dst_ref=ar.at[t],
                send_sem=asend.at[i], recv_sem=arecv.at[t],
                device_id=(s, q), device_id_type=MESH,
            ).start()
        if i == 0:
            @pl.when(s == 0)
            def _():
                kvb[0:WINDOW, :] = jnp.zeros((WINDOW, kvb.shape[1]), BF16)
                g[0:HALO, :] = jnp.zeros((HALO, CC), BF16)

            @pl.when(s > 0)
            def _():
                halo(kvb, WINDOW, 0).wait_recv()
                halo(g, HALO, 1).wait_recv()

            send_gated(0)
            for r, cond in ((1, None), (2, mid)):
                plane_w(r, W0, cond)
                relay(r, W0)
            relay(1, N)
        elif i == 1:
            for u in M:
                to_x(None, s, u)
        elif i == 2:
            for r, cond in ((1, None), (2, mid)):
                plane_w(r, W1, cond)
                relay(r, W1)
    own_rows = pl.multiple_of(t * Q, Q)
    ar[t] = a[pl.ds(own_rows, Q), :]
    gr[t] = g[pl.ds(own_rows, HALO + Q), :]
    other_n(1, mid)
    relay(1, N, True)
    across(mine(1))
    for u in M:
        relay(1, u)

    first = HALO - (CONV_WIDTH - 1)
    for j in range(T):
        k, b = j // 2, j % 2
        p = 2 * lax.rem(y + k, Y) + (c if b == 0 else 1 - c)
        if j > 0:
            pltpu.make_async_copy(gr.at[p], gr.at[p], grecv.at[p]).wait()
        cols = pl.ds(pl.multiple_of(p * CC, CC), CC)
        ext[j] = gr[p].astype(F32)
        total = jnp.zeros((Q, CC), F32)
        tp = taps[:, cols].astype(F32)
        for k in range(CONV_WIDTH):
            total = total + tp[k : k + 1] * ext[j, first + k : first + k + Q, :]
        conv[:, cols] = total.astype(BF16)
        if j == 1:
            plane_n(2, end)
            inner()
            plane_w(last, W0, mid)
            relay(last, W0)
            other_n(1, end)
            other_n(2, mid)
            plane_n(last, mid)
            relay(last, N)
        elif j == 2:
            plane_w(2, W0, end)
    plane_w(last, W1, mid)
    relay(last, W1)
    plane_w(2, W1, end)
    cv = conv[...].astype(F32)
    cen = cv - jnp.mean(cv, axis=-1, keepdims=True)
    norm = cen * lax.rsqrt(jnp.mean(cen * cen, axis=-1, keepdims=True) + EPS) * cg[...]
    act[...] = (norm * jax.nn.sigmoid(norm)).astype(BF16)
    loads[6].wait()
    pt = jnp.dot(act[...], pw[...], preferred_element_type=F32)
    AW = T * HW

    def swap(lo, hi, i):
        pltpu.make_async_remote_copy(
            src_ref=mg.at[0:Q, lo:hi], dst_ref=mg.at[Q : 2 * Q, lo:hi],
            send_sem=msend.at[i], recv_sem=mrecv.at[i],
            device_id=(s, sib), device_id_type=MESH,
        ).start()

    def swapped(lo, hi, i):
        ref = mg.at[Q : 2 * Q, lo:hi]
        pltpu.make_async_copy(ref, ref, mrecv.at[i]).wait()

    mg[0:Q, AW:] = (
        pt * lax.rsqrt(jnp.mean(pt * pt, axis=-1, keepdims=True) + EPS) * og[:, AW:]
    ).astype(BF16)
    swap(AW, mg.shape[1], 1)
    plane_w(last, W0, end)
    other_n(last, mid)
    relay(last, N, True)
    across(mine(last), mid)
    for u in M:
        relay(last, u)
    for d in range(1, T):
        p = lax.rem(t + d, T)
        pltpu.make_async_copy(ar.at[p], ar.at[p], arecv.at[p]).wait()
    heads = jnp.concatenate([ar[p] for p in range(T)], axis=1).astype(F32)
    mg[0:Q, :AW] = (
        heads * lax.rsqrt(jnp.mean(heads * heads, axis=-1, keepdims=True) + EPS) * og[:, :AW]
    ).astype(BF16)

    swap(0, AW, 0)

    nb = D // 8
    K2 = 2 * Kl
    tiled = K2 % 128 == 0
    upper, lower = slice(0, Q), slice(Q, 2 * Q)

    def term(r, rows, cols):
        ks = pl.ds(pl.multiple_of(plane(r) * K2, K2), K2)
        return jnp.dot(mg[rows, ks], wfull[ks, cols], preferred_element_type=F32)

    def blocks():
        return [slice(n * nb, (n + 1) * nb) for n in range(half // nb)]

    other_n(2, end)
    plane_n(last, end)
    other_n(0)
    other_w(0)
    across(other(0))
    rest(1)
    plane_w(last, W1, end)
    swapped(AW, mg.shape[1], 1)
    swapped(0, AW, 0)
    if tiled:
        for cols in blocks():
            acc[:, cols] = term(0, slice(None), cols) + term(1, slice(None), cols)
    other_n(last, end)
    rest(2)
    if tiled:
        for r in range(2, Z - 1):
            for cols in blocks():
                acc[:, cols] += term(r, slice(None), cols)
    def total(rows, cols):
        if tiled:
            return (acc[rows, cols] + term(Z - 1, rows, cols)).astype(BF16)
        return jnp.dot(mg[rows, :], wfull[:, cols], preferred_element_type=F32).astype(BF16)

    def landing(cc, cols):
        start = pl.multiple_of(cc * half + cols.start, nb)
        return out.at[:, pl.ds(start, cols.stop - cols.start)]

    outs = []

    def finish(cols):
        i = len(outs)
        both = total(slice(None), cols)
        theirs[:, cols] = both[lower]
        landing(c, cols)[...] = both[upper]
        copy = pltpu.make_async_remote_copy(
            src_ref=theirs.at[:, cols], dst_ref=landing(c, cols),
            send_sem=osend.at[i], recv_sem=orecv.at[i],
            device_id=(s, sib), device_id_type=MESH,
        )
        copy.start()
        outs.append((copy, cols))

    across(mine(last), end)
    across(other(last))
    if not tiled:
        other_w(Z - 1)
    finish(slice(wide, half))
    for u in (W0, W1):
        if tiled:
            got(None, other(Z - 1), u)
        finish(slice(u * part, (u + 1) * part))
    drain()

    @pl.when(s + 1 < S)
    def _():
        halo(kvb, WINDOW, 0).wait_send()
        halo(g, HALO, 1).wait_send()

    for q in range(T):
        @pl.when(t != q)
        def _():
            pltpu.make_async_copy(gr.at[0], gr.at[0], gsend.at[q]).wait()
    for i in range(T - 1):
        pltpu.make_async_copy(ar.at[0], ar.at[0], asend.at[i]).wait()
    for i, (lo, hi) in enumerate(((0, AW), (AW, mg.shape[1]))):
        ref = mg.at[0:Q, lo:hi]
        pltpu.make_async_copy(ref, ref, msend.at[i]).wait()
    for i, (copy, cols) in enumerate(outs):
        copy.wait_send()
        ref = landing(1 - c, cols)
        pltpu.make_async_copy(ref, ref, orecv.at[i]).wait()


def solution(mesh):
    S, T = mesh.shape["sp"], mesh.shape["tp"]

    def step(
        tokens, norm_gain, query_weight, key_weight, value_weight, sink_logits, conv_in_weight,
        conv_gate_weight, conv_taps, conv_gain, point_weight, output_gain, output_weight,
    ):
        R, D = tokens.shape
        Q = R // T
        HW, KW, CC = query_weight.shape[1], key_weight.shape[1], conv_in_weight.shape[1]
        C = point_weight.shape[0]
        MIX = output_gain.shape[0]
        Y, Z = T // 2, S // 2
        hbm = pl.BlockSpec(memory_space=pl.ANY)
        vmem = pl.BlockSpec(memory_space=pltpu.VMEM)
        dma = pltpu.SemaphoreType.DMA
        return pl.pallas_call(
            functools.partial(kernel, S, T),
            out_shape=pltpu.VMEM((Q, D), BF16),
            in_specs=[hbm] * 13,
            out_specs=vmem,
            scratch_shapes=[
                pltpu.VMEM((R, D), BF16),
                pltpu.VMEM((D, HW + 2 * KW + 2 * CC), BF16),
                pltpu.VMEM((2 * KW, D), BF16),
                pltpu.VMEM((C, C), BF16),
                pltpu.VMEM((MIX, D // 2), BF16),
                pltpu.VMEM((R, HW), BF16),
                pltpu.VMEM((R + WINDOW, 2 * KW), BF16),
                pltpu.VMEM((R + HALO, CC), BF16),
                pltpu.VMEM((R, HW), BF16),
                pltpu.VMEM((T, Q, HW), BF16),
                pltpu.VMEM((T, Q + HALO, CC), BF16),
                pltpu.VMEM((T, Q + HALO, CC), F32),
                pltpu.VMEM((Q, C), BF16),
                pltpu.VMEM((Q, C), BF16),
                pltpu.VMEM((2 * Q, MIX), BF16),
                pltpu.VMEM((2 * Q, D // 2), F32),
                pltpu.VMEM((Q, D // 2), BF16),
                pltpu.VMEM((1, D), F32),
                pltpu.SMEM(sink_logits.shape, F32),
                pltpu.VMEM(conv_taps.shape, BF16),
                pltpu.VMEM((1, C), F32),
                pltpu.VMEM((1, MIX), F32),
                dma((12 + T,)),
                dma((8 * Z + 16,)),
                dma((S, Y + 2)),
                dma((2,)),
                dma((2,)),
                dma((T,)),
                dma((T,)),
                dma((T,)),
                dma((T,)),
                dma((2,)),
                dma((2,)),
                dma((4,)),
                dma((4,)),
            ],
            compiler_params=pltpu.CompilerParams(
                collective_id=0, has_side_effects=True, vmem_limit_bytes=56 * 1024 * 1024
            ),
        )(
            tokens, norm_gain[None], query_weight, key_weight.T, value_weight.T, sink_logits,
            conv_in_weight, conv_gate_weight, conv_taps, conv_gain[None], point_weight,
            output_gain[None], output_weight,
        )

    in_specs = (
        P("sp", None), P(), P(None, "tp"), P(None, "tp"), P(None, "tp"), P("tp"), P(None, "tp"),
        P(None, "tp"), P(), P(), P(), P(), P("sp", None),
    )
    return jax.shard_map(
        step, mesh=mesh, in_specs=in_specs, out_specs=P(("sp", "tp"), None), check_vma=False
    )
```
